32 devices in a mesh: grp: 2 (over y), ep: 4 (over z), tp: 4 (over x, core).
Axes of the slice: x: 2, y: 2, z: 4, core: 2. Of those that a mesh axis runs over, the one named last changes fastest.
Arguments:
- queries: bfloat16 [1024, 1024], P(('grp', 'ep'), 'tp'), parts along dimension 0, may hold values from -6 to 6
- keys: bfloat16 [1024, 1024], P(('grp', 'ep'), 'tp'), parts along dimension 0, may hold values from -6 to 6
- values: bfloat16 [1024, 1024], P(('grp', 'ep'), 'tp'), parts along dimension 0, may hold values from -6 to 6
- lambdas: float32 [8], P('tp'), may hold values from 0.3 to 0.8
- head_gain: float32 [128], replicated, may hold values from 0.1 to 1.9
- tokens: bfloat16 [2048, 1536], P(('grp', 'ep')), parts along dimension 0, may hold values from -6 to 6
- route_ids: int32 [2048, 2], P(('grp', 'ep')), parts along dimension 0, may hold values from 0 to 3, all different within a row; in each aligned block of 256 rows (0 to 255, 256 to 511, ...) at most 256 rows name the same one
- route_weights: float32 [2048, 2], P(('grp', 'ep')), parts along dimension 0, may hold values from 0.2 to 1
- moe_gain: float32 [1536], replicated, may hold values from 0.1 to 1.9
- w_gate: bfloat16 [4, 1536, 3072], P('ep', None, 'tp'), may hold values from -0.15625 to 0.15625
- w_up: bfloat16 [4, 1536, 3072], P('ep', None, 'tp'), may hold values from -0.15625 to 0.15625
- w_down: bfloat16 [4, 3072, 1536], P('ep', 'tp'), may hold values from -0.109375 to 0.109375
Outputs:
- heads_out: bfloat16 [1024, 1024], P(('grp', 'ep'), 'tp'), parts along dimension 0
- expert_out: bfloat16 [2048, 1536], P(('grp', 'ep'), 'tp'), parts along dimension 0
The draws below stay inside these ranges and needn't reach their ends.
There are 2 independent parts, one for each index of `grp`. The reference program is written for one: setup_inputs(seed, part) draws one part's arguments, and reference() takes and returns one part's arrays. A program takes and returns all parts, laid end to end along the dimension named above; an argument that names none is the same for every part. Nothing has to cross between parts.
Inputs may be any that keep to these rules, and one draw needn't show every extreme that they name: `route_ids`: each row names 2 different experts. In the 256 rows of one device no expert is named more than 256 times, and in every draw some device names some expert exactly 256 times.
All inputs are finite; a program needn't handle non-finite values.
Results may differ from the reference program's by a relative error of at most 0.015.
Values may be sent and summed in bfloat16 or wider, within the bound.
No kernel may reach another device: no remote copies, remote signals or barrier semaphores. Data moves between devices by JAX's collectives and lax.ppermute only.
A program may use at most 64 MiB of HBM per device.

```python
import math
import jax
import jax.numpy as jnp
import numpy as np
from jax import lax

D = 1536
FF = 3072
HEADS = 8
HEAD_DIM = 64
VALUE_DIM = 128
TOP = 2
ROW_DEV = 256
EXPERTS = 4
CAP = 256
SEQ = 512
ROWS = 1024
N_EP = 4
N_TP = 4


def draw_pair(key):
    base = jax.random.fold_in(key, 17)
    width = HEADS * 2 * HEAD_DIM
    query_key, key_key = jax.random.split(base, 2)
    query_field = jnp.clip(jax.random.normal(query_key, (SEQ, width), jnp.float32) * 1.33, -6.0, 6.0)
    key_field = jnp.clip(jax.random.normal(key_key, (SEQ, width), jnp.float32) * 1.33, -6.0, 6.0)
    return (query_field, key_field)


def draw_queries(key, part):
    return draw_pair(key)[0].astype(jnp.bfloat16)


def draw_keys(key, part):
    return draw_pair(key)[1].astype(jnp.bfloat16)


def block_scale(own_key, extent, pieces, smallest, largest):
    factor_of = 1.0
    for dim, blocks in pieces:
        heights = jax.random.uniform(jax.random.fold_in(jax.random.fold_in(own_key, 6), dim), (blocks,), jnp.float32, smallest / len(pieces), largest / len(pieces))
        factor_of = factor_of * jnp.repeat(jnp.exp(heights), extent[dim] // blocks).reshape((-1,) + (1,) * (len(extent) - 1 - dim))
    return factor_of


def deal_out(own_key, own, number, rows, amount, top, most, slope):
    ranking = jax.random.permutation(own_key, amount)
    heavy_load, usual = shares(amount, rows * top, most, slope, True), shares(amount, rows * top, most, slope, False)
    places = jnp.arange(amount)

    def named(sizes, offset_by):
        used = int((sizes > 0).sum())
        fixed = max(1, used // 4)
        moved = fixed + (places - fixed + offset_by * (used - fixed)) % max(1, amount - fixed)
        return jnp.zeros((amount,), jnp.int32).at[ranking[jnp.where(places < fixed, places, moved)]].set(jnp.asarray(sizes, jnp.int32))

    sizes = jnp.where(number % 4 == 0, named(heavy_load, number // 4), named(usual, number - number // 4 - 1))
    mixed = jax.random.permutation(jax.random.fold_in(own, 3), amount)
    source_of, sink = mixed[0:amount // 2 * 2:2], mixed[1:amount // 2 * 2:2]
    margin = jnp.minimum(sizes[source_of] - 1, most - sizes[sink]) // 2
    margin = jnp.where((source_of == ranking[0]) | (sink == ranking[0]) | (sizes[sink] == 0), 0, jnp.maximum(margin, 0))
    moved = jax.random.randint(jax.random.fold_in(own, 4), (amount // 2,), 0, 1 << 20) % (margin + 1)
    sizes = sizes.at[source_of].add(-moved).at[sink].add(moved)
    items = jnp.searchsorted(jnp.cumsum(sizes), jnp.arange(rows * top), side="right").astype(jnp.int32)
    listing = items.reshape(top, rows).T
    listing = listing[jax.random.permutation(jax.random.fold_in(own, 1), rows)]
    offset_by = jax.random.randint(jax.random.fold_in(own, 2), (rows, 1), 0, top)
    return jnp.take_along_axis(listing, (jnp.arange(top)[None, :] + offset_by) % top, axis=1)


def shares(count, total, bound, slope, full):
    weights = [(1 << 20) // math.isqrt(rank ** slope) + 1 for rank in range(1, count + 1)]
    largest = bound if full else min(bound, max(-(-total // count), total * weights[0] // sum(weights)))
    least = 1 if total - largest >= count - 1 else 0
    counts, surplus = [largest] + [least] * (count - 1), total - largest - least * (count - 1)
    while surplus > 0:
        free = [i for i in range(1, count) if counts[i] < largest] or [i for i in range(1, count) if counts[i] < bound]
        mass, budget = sum([weights[i] for i in free]), surplus
        for i in free:
            more = min(bound - counts[i], max(1, budget * weights[i] // mass), surplus)
            counts[i] = counts[i] + more
            surplus = surplus - more
    return np.array(counts)


def bell_draw(key, dims, spread, limit, shards=(), kind=jnp.bfloat16):
    factor_of = block_scale(key, dims, shards, -0.22, 0.18) if shards else 1.0
    entries = jax.random.normal(key, dims, jnp.float32) * spread * factor_of
    return jnp.minimum(jnp.maximum(entries, -limit), limit).astype(kind)


def setup_inputs(seed: int = 0, part: int = 0) -> dict:
    splits = jax.random.split(jax.random.key(seed), 13)
    own_keys = jax.random.split(jax.random.fold_in(splits[12], part), 13)
    queries = draw_queries(jax.random.fold_in(jax.random.fold_in(splits[12], part), 71), part)
    keys = draw_keys(jax.random.fold_in(jax.random.fold_in(splits[12], part), 71), part)
    values = bell_draw(own_keys[2], (SEQ, HEADS * VALUE_DIM), 1.0, 6.0, ((0, 4), (1, 4)))
    lambdas = jnp.clip(0.3 + 0.5 * jax.random.uniform(splits[3], (HEADS,), jnp.float32) ** block_scale(splits[3], (HEADS,), ((0, 4),), -0.2, 0.2), 0.3, 0.8)
    head_gain = jnp.clip(1.0 + 0.18 * jax.random.normal(splits[4], (VALUE_DIM,), jnp.float32), 0.1, 1.9)
    tokens = bell_draw(own_keys[5], (ROWS, D), 1.0, 6.0, ((0, 4),))
    route_ids_keys = jax.random.split(jax.random.fold_in(own_keys[6], 1), ROWS // ROW_DEV)
    route_ids_turns = jax.random.permutation(jax.random.fold_in(own_keys[6], 3), ROWS // ROW_DEV)
    route_ids = jax.vmap(lambda own, number: deal_out(jax.random.fold_in(own_keys[6], 2), own, number, ROW_DEV, EXPERTS, TOP, CAP, 2))(route_ids_keys, route_ids_turns).reshape((ROWS, TOP))
    route_weights = jnp.clip(0.2 + 0.8 * jax.random.uniform(own_keys[7], (ROWS, TOP), jnp.float32) ** block_scale(own_keys[7], (ROWS, TOP), ((0, 4),), -0.2, 0.2), 0.2, 1.0)
    moe_gain = jnp.clip(1.0 + 0.18 * jax.random.normal(splits[8], (D,), jnp.float32), 0.1, 1.9)
    w_gate = bell_draw(splits[9], (EXPERTS, D, FF), D ** -0.5, 0.15625, ((0, 4), (2, 4)))
    w_up = bell_draw(splits[10], (EXPERTS, D, FF), D ** -0.5, 0.15625, ((0, 4), (2, 4)))
    w_down = bell_draw(splits[11], (EXPERTS, FF, D), FF ** -0.5, 0.109375, ((0, 4), (1, 4)))
    return dict(queries=queries, keys=keys, values=values, lambdas=lambdas, head_gain=head_gain, tokens=tokens, route_ids=route_ids, route_weights=route_weights, moe_gain=moe_gain, w_gate=w_gate, w_up=w_up, w_down=w_down)


def head_mix(operands):
    query_head, key_head, value_head, lambda_head, head_gain = operands
    block = math.gcd(SEQ, 512)
    query_blocks = query_head.reshape(SEQ // block, block, 2, HEAD_DIM)

    def one_block(query_part):
        results = []
        for component in range(2):
            scores = jnp.dot(query_part[:, component], key_head[:, component].T, preferred_element_type=jnp.float32) * HEAD_DIM ** (-0.5)
            highest = lax.optimization_barrier(jnp.max(scores, axis=1, keepdims=True))
            shifted = jnp.exp(scores - highest)
            totals = lax.optimization_barrier(jnp.sum(shifted, axis=1, keepdims=True))
            sums = jnp.dot(shifted.astype(jnp.bfloat16), value_head, preferred_element_type=jnp.float32)
            results.append(sums / totals)
        mixed = results[0] - lambda_head * results[1]
        scaled = mixed * lax.rsqrt(lax.optimization_barrier(jnp.mean(mixed * mixed, axis=1, keepdims=True)) + 1e-06) * head_gain
        return scaled.astype(jnp.bfloat16)
    return lax.map(one_block, query_blocks).reshape(SEQ, VALUE_DIM)

def reference(queries, keys, values, lambdas, head_gain, tokens, route_ids, route_weights, moe_gain, w_gate, w_up, w_down):
    query_heads = jnp.transpose(queries.reshape(SEQ, HEADS, 2, HEAD_DIM), (1, 0, 2, 3))
    key_heads = jnp.transpose(keys.reshape(SEQ, HEADS, 2, HEAD_DIM), (1, 0, 2, 3))
    value_heads = jnp.transpose(values.reshape(SEQ, HEADS, VALUE_DIM), (1, 0, 2))
    gains = jnp.broadcast_to(head_gain, (HEADS, VALUE_DIM))
    mixed_heads = lax.map(head_mix, (query_heads, key_heads, value_heads, lambdas, gains))
    heads_out = jnp.transpose(mixed_heads, (1, 0, 2)).reshape(SEQ, HEADS * VALUE_DIM)
    token_float = tokens.astype(jnp.float32)
    normed = (token_float * lax.rsqrt(lax.optimization_barrier(jnp.mean(token_float * token_float, axis=1, keepdims=True)) + 1e-06) * moe_gain).astype(jnp.bfloat16)
    flat_ids = route_ids.reshape(N_EP, ROW_DEV * TOP)
    onehot = (flat_ids[:, :, None] == jnp.arange(EXPERTS, dtype=jnp.int32)[None, None, :]).astype(jnp.int32)
    earlier = jnp.cumsum(onehot, axis=1) - onehot
    position = lax.optimization_barrier(jnp.sum(earlier * onehot, axis=2)).astype(jnp.int32)
    source = jnp.broadcast_to(jnp.arange(N_EP, dtype=jnp.int32)[:, None], (N_EP, ROW_DEV * TOP))
    owner_row = source * ROW_DEV + jnp.arange(ROW_DEV * TOP, dtype=jnp.int32)[None, :] // TOP
    table = jnp.full((EXPERTS, N_EP, CAP), ROWS, jnp.int32).at[flat_ids, source, position].set(owner_row)
    padded = jnp.concatenate([normed, jnp.zeros((1, D), jnp.bfloat16)], axis=0)

    def expert_pass(operands):
        rows_index, gate_mat, up_mat, down_mat = operands
        arrived = padded[rows_index.reshape(-1)]
        gate = jnp.dot(arrived, gate_mat, preferred_element_type=jnp.float32)
        upward = jnp.dot(arrived, up_mat, preferred_element_type=jnp.float32)
        hidden = (jax.nn.silu(gate) * upward).astype(jnp.bfloat16)
        hidden_blocks = jnp.transpose(hidden.reshape(-1, N_TP, FF // N_TP), (1, 0, 2)).astype(jnp.float32)
        down_blocks = down_mat.reshape(N_TP, FF // N_TP, D).astype(jnp.float32)
        partial_sums = jnp.einsum('jsf,jfd->jsd', hidden_blocks, down_blocks)
        rounded = lax.optimization_barrier(partial_sums.astype(jnp.bfloat16))
        return lax.optimization_barrier(jnp.sum(rounded.astype(jnp.float32), axis=0)).astype(jnp.bfloat16)
    results = lax.map(expert_pass, (table, w_gate, w_up, w_down)).reshape(EXPERTS, N_EP, CAP, D)
    picked = results[flat_ids, source, position].reshape(ROWS, TOP, D).astype(jnp.float32)
    expert_out = jnp.einsum('rkd,rk->rd', picked, route_weights).astype(jnp.bfloat16)
    return (heads_out, expert_out)
```

```python
import jax
import jax.numpy as jnp
from jax import lax
from jax.sharding import PartitionSpec as P


def xor_pairs(size, step):
    return [(i, i ^ step) for i in range(size)]


def halving_steps(size):
    steps = []
    step = size // 2
    while step >= 1:
        steps.append(step)
        step //= 2
    return steps


def power_of_two(size):
    return size & (size - 1) == 0


def gathered(piece):
    size = lax.axis_size("ep")
    pieces = [piece]
    for step in range(1, size):
        pieces.append(lax.ppermute(piece, "ep", xor_pairs(size, step)))
    return jnp.concatenate(pieces, axis=0)


def attend(queries, keys, values, lambdas, head_gain):
    row_count = queries.shape[0]
    head_count = lambdas.shape[0]
    head_dim = queries.shape[1] // (2 * head_count)
    value_dim = values.shape[1] // head_count
    query_parts = queries.reshape(row_count, head_count, 2, head_dim)
    score_scale = head_dim ** (-0.5)
    if power_of_two(lax.axis_size("ep")) and lax.axis_size("ep") <= 4:
        both = gathered(jnp.concatenate([keys, values], axis=1))
        key_piece, value_piece = both[:, : keys.shape[1]], both[:, keys.shape[1] :]
    else:
        key_piece = lax.all_gather(keys, "ep", axis=0, tiled=True)
        value_piece = lax.all_gather(values, "ep", axis=0, tiled=True)
    count = key_piece.shape[0]
    key_parts = key_piece.reshape(count, head_count, 2, head_dim)
    value_parts = value_piece.reshape(count, head_count, value_dim)
    scores = (
        jnp.einsum("qhcd,khcd->hcqk", query_parts, key_parts, preferred_element_type=jnp.float32)
        * score_scale
    )
    newest = jnp.max(scores, axis=-1)
    weights_now = jnp.exp(scores - newest[..., None])
    totals = jnp.sum(weights_now, axis=-1)
    sums = jnp.einsum(
        "hcqk,khe->hcqe",
        weights_now.astype(jnp.bfloat16),
        value_parts,
        preferred_element_type=jnp.float32,
    )
    means = sums / totals[..., None]
    mixed = means[:, 0] - lambdas[:, None, None] * means[:, 1]
    scaled = mixed * lax.rsqrt(jnp.mean(mixed * mixed, axis=-1, keepdims=True) + 1e-06) * head_gain
    return (
        jnp.transpose(scaled, (1, 0, 2))
        .reshape(row_count, head_count * value_dim)
        .astype(jnp.bfloat16)
    )


def normalize(tokens, moe_gain):
    token_float = tokens.astype(jnp.float32)
    return (
        token_float
        * lax.rsqrt(jnp.mean(token_float * token_float, axis=1, keepdims=True) + 1e-06)
        * moe_gain
    ).astype(jnp.bfloat16)


def experts_whole(tokens, route_ids, route_weights, moe_gain, w_gate, w_up, w_down):
    row_count, width = tokens.shape
    ep_size = lax.axis_size("ep")
    tp_size = lax.axis_size("tp")
    ep_index = lax.axis_index("ep")
    tp_index = lax.axis_index("tp")
    steps = halving_steps(tp_size)
    piece_rows = row_count // tp_size
    part = jnp.zeros((), jnp.int32)
    for place, step in enumerate(steps):
        part = part + jnp.where(tp_index & step != 0, 1 << place, 0)
    mine = normalize(
        lax.dynamic_slice_in_dim(tokens, part * piece_rows, piece_rows, 0), moe_gain
    )
    arrivals = [
        lax.ppermute(mine, "ep", xor_pairs(ep_size, step)) for step in range(1, ep_size)
    ]
    gate_mat, up_mat = w_gate[0], w_up[0]
    slice_width = width // tp_size
    order = []
    for place in range(tp_size):
        target = tp_index
        for bit, step in enumerate(steps):
            if not (place >> bit) & 1:
                target = target ^ step
        order.append(target)
    down_mat = jnp.concatenate(
        [lax.dynamic_slice_in_dim(w_down[0], t * slice_width, slice_width, 1) for t in order],
        axis=1,
    )

    def all_rows(piece):
        for step in steps:
            other = lax.ppermute(piece, "tp", xor_pairs(tp_size, step))
            low = tp_index & step == 0
            piece = jnp.concatenate(
                [jnp.where(low, piece, other), jnp.where(low, other, piece)], axis=0
            )
        return piece

    def expert(rows):
        gate = jnp.dot(rows, gate_mat, preferred_element_type=jnp.float32)
        upward = jnp.dot(rows, up_mat, preferred_element_type=jnp.float32)
        hidden = (jax.nn.silu(gate) * upward).astype(jnp.bfloat16)
        partial = jnp.dot(hidden, down_mat, preferred_element_type=jnp.float32).astype(
            jnp.bfloat16
        )
        for step in reversed(steps):
            half = partial.shape[1] // 2
            other = lax.ppermute(partial[:, :half], "tp", xor_pairs(tp_size, step))
            partial = (
                partial[:, half:].astype(jnp.float32) + other.astype(jnp.float32)
            ).astype(jnp.bfloat16)
        return partial

    results = [expert(normalize(tokens, moe_gain))]
    for step in range(1, ep_size):
        done = expert(all_rows(arrivals[step - 1]))
        results.append(lax.ppermute(done, "ep", xor_pairs(ep_size, step)))
    total = jnp.zeros((row_count, slice_width), jnp.float32)
    for step in range(ep_size):
        named = route_ids == (ep_index ^ step)
        weight = jnp.sum(jnp.where(named, route_weights, 0.0), axis=1, keepdims=True)
        here = jnp.any(named, axis=1, keepdims=True)
        total = total + jnp.where(here, results[step].astype(jnp.float32) * weight, 0.0)
    return total.astype(jnp.bfloat16)


def experts_slots(tokens, route_ids, route_weights, moe_gain, w_gate, w_up, w_down):
    row_count, width = tokens.shape
    top_count = route_ids.shape[1]
    ep_size = lax.axis_size("ep")
    tp_size = lax.axis_size("tp")
    expert_count = w_gate.shape[0] * ep_size
    capacity = 2 * row_count * top_count // expert_count
    normed = normalize(tokens, moe_gain)
    flat_ids = route_ids.reshape(-1)
    onehot = (flat_ids[:, None] == jnp.arange(expert_count, dtype=jnp.int32)[None, :]).astype(
        jnp.int32
    )
    earlier = jnp.cumsum(onehot, axis=0) - onehot
    position = jnp.sum(earlier * onehot, axis=1)
    slot_index = flat_ids * capacity + position
    owners = (
        jnp.full((expert_count * capacity,), row_count, jnp.int32)
        .at[slot_index]
        .set(jnp.arange(row_count * top_count, dtype=jnp.int32) // top_count)
    )
    padded = jnp.concatenate([normed, jnp.zeros((1, width), jnp.bfloat16)], axis=0)
    outgoing = padded[owners].reshape(expert_count, capacity, width)
    gate_mat = w_gate[0]
    up_mat = w_up[0]
    down_mat = w_down[0]
    slice_width = width // tp_size
    own_columns = lax.dynamic_slice_in_dim(
        outgoing, lax.axis_index("tp") * slice_width, slice_width, 2
    )
    arrived = lax.all_to_all(own_columns, "ep", split_axis=0, concat_axis=0, tiled=True)
    piece = lax.all_gather(arrived, "tp", axis=2, tiled=True)
    gate = jnp.einsum("scd,df->scf", piece, gate_mat, preferred_element_type=jnp.float32)
    upward = jnp.einsum("scd,df->scf", piece, up_mat, preferred_element_type=jnp.float32)
    hidden = (jax.nn.silu(gate) * upward).astype(jnp.bfloat16)
    flat_hidden = hidden.reshape(-1, hidden.shape[2])
    summed = lax.psum_scatter(
        jnp.einsum("fd,sf->ds", down_mat, flat_hidden, preferred_element_type=jnp.float32).astype(
            jnp.bfloat16
        ),
        "tp",
        scatter_dimension=0,
        tiled=True,
    )
    back = lax.all_to_all(summed, "ep", split_axis=1, concat_axis=1, tiled=True)
    picked = (
        jnp.take(back, slot_index, axis=1).astype(jnp.float32).reshape(-1, row_count, top_count)
    )
    combined = jnp.einsum("drk,rk->rd", picked, route_weights)
    return combined.astype(jnp.bfloat16)


def experts(tokens, route_ids, route_weights, moe_gain, w_gate, w_up, w_down):
    row_count = tokens.shape[0]
    ep_size = lax.axis_size("ep")
    tp_size = lax.axis_size("tp")
    expert_count = w_gate.shape[0] * ep_size
    capacity = 2 * row_count * route_ids.shape[1] // expert_count
    whole = (
        capacity >= row_count
        and w_gate.shape[0] == 1
        and power_of_two(ep_size)
        and power_of_two(tp_size)
        and row_count % tp_size == 0
    )
    chosen = experts_whole if whole else experts_slots
    return chosen(tokens, route_ids, route_weights, moe_gain, w_gate, w_up, w_down)


def on_device(
    queries,
    keys,
    values,
    lambdas,
    head_gain,
    tokens,
    route_ids,
    route_weights,
    moe_gain,
    w_gate,
    w_up,
    w_down,
):
    heads_out = attend(queries, keys, values, lambdas, head_gain)
    expert_out = experts(tokens, route_ids, route_weights, moe_gain, w_gate, w_up, w_down)
    return (heads_out, expert_out)


def solution(mesh):
    in_specs = (
        P(("grp", "ep"), "tp"),
        P(("grp", "ep"), "tp"),
        P(("grp", "ep"), "tp"),
        P("tp"),
        P(),
        P(("grp", "ep"), None),
        P(("grp", "ep"), None),
        P(("grp", "ep"), None),
        P(),
        P("ep", None, "tp"),
        P("ep", None, "tp"),
        P("ep", "tp", None),
    )
    out_specs = (P(("grp", "ep"), "tp"), P(("grp", "ep"), "tp"))
    return jax.shard_map(
        on_device, mesh=mesh, in_specs=in_specs, out_specs=out_specs, check_vma=False
    )
```

```python
import math

import jax
import jax.numpy as jnp
from jax import lax
from jax.experimental import pallas as pl
from jax.experimental.pallas import tpu as pltpu
from jax.sharding import PartitionSpec as P


def xor_pairs(size, step):
    return [(i, i ^ step) for i in range(size)]


def halving_steps(size):
    steps = []
    step = size // 2
    while step >= 1:
        steps.append(step)
        step //= 2
    return steps


def power_of_two(size):
    return size & (size - 1) == 0


def gathered(piece):
    size = lax.axis_size("ep")
    pieces = [piece]
    for step in range(1, size):
        pieces.append(lax.ppermute(piece, "ep", xor_pairs(size, step)))
    return jnp.concatenate(pieces, axis=0)


def attend(queries, keys, values, lambdas, head_gain):
    row_count = queries.shape[0]
    head_count = lambdas.shape[0]
    head_dim = queries.shape[1] // (2 * head_count)
    value_dim = values.shape[1] // head_count
    query_parts = queries.reshape(row_count, head_count, 2, head_dim)
    score_scale = head_dim ** (-0.5)
    if power_of_two(lax.axis_size("ep")) and lax.axis_size("ep") <= 4:
        both = gathered(jnp.concatenate([keys, values], axis=1))
        key_piece, value_piece = both[:, : keys.shape[1]], both[:, keys.shape[1] :]
    else:
        key_piece = lax.all_gather(keys, "ep", axis=0, tiled=True)
        value_piece = lax.all_gather(values, "ep", axis=0, tiled=True)
    count = key_piece.shape[0]
    key_parts = key_piece.reshape(count, head_count, 2, head_dim)
    value_parts = value_piece.reshape(count, head_count, value_dim)
    scores = (
        jnp.einsum("qhcd,khcd->hcqk", query_parts, key_parts, preferred_element_type=jnp.float32)
        * score_scale
    )
    newest = jnp.max(scores, axis=-1)
    weights_now = jnp.exp(scores - newest[..., None])
    totals = jnp.sum(weights_now, axis=-1)
    sums = jnp.einsum(
        "hcqk,khe->hcqe",
        weights_now.astype(jnp.bfloat16),
        value_parts,
        preferred_element_type=jnp.float32,
    )
    means = sums / totals[..., None]
    mixed = means[:, 0] - lambdas[:, None, None] * means[:, 1]
    scaled = mixed * lax.rsqrt(jnp.mean(mixed * mixed, axis=-1, keepdims=True) + 1e-06) * head_gain
    return (
        jnp.transpose(scaled, (1, 0, 2))
        .reshape(row_count, head_count * value_dim)
        .astype(jnp.bfloat16)
    )


def normalize(tokens, moe_gain):
    token_float = tokens.astype(jnp.float32)
    return (
        token_float
        * lax.rsqrt(jnp.mean(token_float * token_float, axis=1, keepdims=True) + 1e-06)
        * moe_gain
    ).astype(jnp.bfloat16)


def rms_rows(token_block, gain_row):
    token_float = token_block.astype(jnp.float32)
    scale = lax.rsqrt(jnp.mean(token_float * token_float, axis=1, keepdims=True) + 1e-06)
    return (token_float * scale * gain_row).astype(jnp.bfloat16)


def call(kernel, name, inputs, spaces, out_shapes, scratch, flops, grant):
    moved = sum(x.size * x.dtype.itemsize for x in inputs)
    moved += sum(math.prod(o.shape) * o.dtype.itemsize for o in out_shapes)
    return pl.pallas_call(
        kernel,
        name=name,
        out_shape=out_shapes,
        in_specs=[pl.BlockSpec(memory_space=s) for s in spaces],
        out_specs=[pl.BlockSpec(memory_space=pltpu.VMEM)] * len(out_shapes),
        scratch_shapes=scratch,
        cost_estimate=pl.CostEstimate(flops=flops, bytes_accessed=moved, transcendentals=0),
        compiler_params=pltpu.CompilerParams(vmem_limit_bytes=grant),
    )(*inputs)


def own_piece(tokens, part, moe_gain, piece_rows):
    width = tokens.shape[1]

    def kernel(part_ref, token_ref, gain_ref, out_ref):
        at = pl.multiple_of(part_ref[0] * piece_rows, piece_rows)
        out_ref[...] = rms_rows(token_ref[pl.ds(at, piece_rows), :], gain_ref[...])

    return call(
        kernel,
        "own_piece",
        (part.reshape(1), tokens, moe_gain.reshape(1, width)),
        (pltpu.SMEM, pltpu.VMEM, pltpu.VMEM),
        [jax.ShapeDtypeStruct((piece_rows, width), jnp.bfloat16)],
        [],
        8 * piece_rows * width,
        4 << 20,
    )[0]


def expert_kernel(pieces, places, blocks, gain, mats, name):
    gate_mat, up_mat, down_mat = mats
    width, units = gate_mat.shape
    block_count = blocks.shape[0]
    block = width // block_count
    part_rows = pieces[0].shape[0]
    row_count = part_rows * len(pieces)
    half = block_count // 2
    chunk = math.gcd(units, 256)

    def kernel(*refs):
        place_ref, block_ref = refs[:2]
        rest = refs[2:]
        if gain is not None:
            gain_ref, rest = rest[0], rest[1:]
        piece_refs, rest = rest[: len(pieces)], rest[len(pieces) :]
        gate_ref, up_ref, down_ref, send_ref, keep_ref, rows, hidden = rest
        if gain is not None:
            rows[...] = rms_rows(piece_refs[0][...], gain_ref[...])
        else:
            for index, ref in enumerate(piece_refs):
                at = pl.multiple_of(place_ref[index] * part_rows, part_rows)
                rows[pl.ds(at, part_rows), :] = ref[...]
        for step in range(units // chunk):
            columns = pl.ds(step * chunk, chunk)
            gate = jnp.dot(rows[...], gate_ref[:, columns], preferred_element_type=jnp.float32)
            upward = jnp.dot(rows[...], up_ref[:, columns], preferred_element_type=jnp.float32)
            hidden[:, columns] = (gate / (1.0 + jnp.exp(-gate)) * upward).astype(jnp.bfloat16)
        for index in range(block_count):
            columns = pl.ds(pl.multiple_of(block_ref[index] * block, block), block)
            out = jnp.dot(
                hidden[...], down_ref[:, columns], preferred_element_type=jnp.float32
            ).astype(jnp.bfloat16)
            if index < half:
                send_ref[:, index * block : (index + 1) * block] = out
            else:
                keep_ref[:, (index - half) * block : (index - half + 1) * block] = out

    gains = () if gain is None else (gain.reshape(1, width),)
    inputs = (places, blocks, *gains, *pieces, gate_mat, up_mat, down_mat)
    spaces = (pltpu.SMEM,) * 2 + (pltpu.VMEM,) * (len(inputs) - 2)
    shape = jax.ShapeDtypeStruct((row_count, half * block), jnp.bfloat16)
    return call(
        kernel,
        name,
        inputs,
        spaces,
        [shape, shape],
        [pltpu.VMEM((row_count, width), jnp.bfloat16), pltpu.VMEM((row_count, units), jnp.bfloat16)],
        6 * row_count * width * units,
        20 << 20,
    )


def add_halves(kept, came, name):
    row_count, columns = kept.shape
    half = columns // 2

    def kernel(kept_ref, came_ref, send_ref, keep_ref):
        for ref, at in ((send_ref, 0), (keep_ref, half)):
            one = kept_ref[:, at : at + half].astype(jnp.float32)
            two = came_ref[:, at : at + half].astype(jnp.float32)
            ref[...] = (one + two).astype(jnp.bfloat16)

    shape = jax.ShapeDtypeStruct((row_count, half), jnp.bfloat16)
    return call(
        kernel,
        name,
        (kept, came),
        (pltpu.VMEM,) * 2,
        [shape, shape],
        [],
        row_count * columns,
        4 << 20,
    )


def add_last(kept, came, name):
    def kernel(kept_ref, came_ref, out_ref):
        out_ref[...] = (
            kept_ref[...].astype(jnp.float32) + came_ref[...].astype(jnp.float32)
        ).astype(jnp.bfloat16)

    return call(
        kernel,
        name,
        (kept, came),
        (pltpu.VMEM,) * 2,
        [jax.ShapeDtypeStruct(kept.shape, jnp.bfloat16)],
        [],
        kept.size,
        4 << 20,
    )[0]


def weighted_sum(route_ids, route_weights, ep_index, own, results):
    row_count, columns = results[0].shape
    top_count = route_ids.shape[1]

    def kernel(index_ref, id_ref, weight_ref, kept_ref, came_ref, *refs):
        result_refs, out_ref = refs[:-1], refs[-1]
        total = jnp.zeros((row_count, columns), jnp.float32)
        for step in range(len(results) + 1):
            expert = index_ref[0] ^ step
            if step == 0:
                result = kept_ref[...].astype(jnp.float32) + came_ref[...].astype(jnp.float32)
                result = result.astype(jnp.bfloat16).astype(jnp.float32)
            else:
                result = result_refs[step - 1][...].astype(jnp.float32)
            for choice in range(top_count):
                named = id_ref[:, choice : choice + 1] == expert
                term = result * weight_ref[:, choice : choice + 1]
                total += jnp.where(named, term, 0.0)
        out_ref[...] = total.astype(jnp.bfloat16)

    inputs = (ep_index.reshape(1), route_ids, route_weights, *own, *results)
    return call(
        kernel,
        "weighted_sum",
        inputs,
        (pltpu.SMEM,) + (pltpu.VMEM,) * (len(inputs) - 1),
        [jax.ShapeDtypeStruct((row_count, columns), jnp.bfloat16)],
        [],
        8 * row_count * columns,
        8 << 20,
    )[0]


def experts_whole(tokens, route_ids, route_weights, moe_gain, w_gate, w_up, w_down):
    row_count, width = tokens.shape
    ep_size = lax.axis_size("ep")
    tp_size = lax.axis_size("tp")
    ep_index = lax.axis_index("ep")
    tp_index = lax.axis_index("tp")
    steps = halving_steps(tp_size)
    piece_rows = row_count // tp_size

    def reversed_bits(index):
        part = jnp.zeros((), jnp.int32)
        for place, step in enumerate(steps):
            part = part + jnp.where(index & step != 0, 1 << place, 0)
        return part

    part = reversed_bits(tp_index)
    mine = own_piece(tokens, part, moe_gain, piece_rows)
    arrivals = [
        lax.ppermute(mine, "ep", xor_pairs(ep_size, step)) for step in range(1, ep_size)
    ]
    mats = (w_gate[0], w_up[0], w_down[0])
    blocks = []
    for place in range(tp_size):
        target = tp_index
        for bit, step in enumerate(steps):
            if not (place >> bit) & 1:
                target = target ^ step
        blocks.append(target)
    blocks = jnp.stack(blocks)

    def all_rows(piece):
        pieces, flips = [piece], [0]
        for step in steps:
            pieces = pieces + [lax.ppermute(p, "tp", xor_pairs(tp_size, step)) for p in pieces]
            flips = flips + [f ^ step for f in flips]
        places = jnp.stack([reversed_bits(tp_index ^ f) for f in flips])
        return pieces, places

    def reduced(send, keep, name, last):
        for step in reversed(steps):
            came = lax.ppermute(send, "tp", xor_pairs(tp_size, step))
            if step == steps[0]:
                return add_last(keep, came, name + "_last") if last else (keep, came)
            send, keep = add_halves(keep, came, name + f"_{step}")

    places = jnp.zeros((1,), jnp.int32)
    own = reduced(
        *expert_kernel([tokens], places, blocks, moe_gain, mats, "expert_0"), "add_0", False
    )
    results = []
    for step in range(1, ep_size):
        pieces, places = all_rows(arrivals[step - 1])
        name = f"expert_{step}"
        done = reduced(*expert_kernel(pieces, places, blocks, None, mats, name), f"add_{step}", True)
        results.append(lax.ppermute(done, "ep", xor_pairs(ep_size, step)))
    return weighted_sum(route_ids, route_weights, ep_index, own, results)


def experts_slots(tokens, route_ids, route_weights, moe_gain, w_gate, w_up, w_down):
    row_count, width = tokens.shape
    top_count = route_ids.shape[1]
    ep_size = lax.axis_size("ep")
    tp_size = lax.axis_size("tp")
    expert_count = w_gate.shape[0] * ep_size
    capacity = 2 * row_count * top_count // expert_count
    normed = normalize(tokens, moe_gain)
    flat_ids = route_ids.reshape(-1)
    onehot = (flat_ids[:, None] == jnp.arange(expert_count, dtype=jnp.int32)[None, :]).astype(
        jnp.int32
    )
    earlier = jnp.cumsum(onehot, axis=0) - onehot
    position = jnp.sum(earlier * onehot, axis=1)
    slot_index = flat_ids * capacity + position
    owners = (
        jnp.full((expert_count * capacity,), row_count, jnp.int32)
        .at[slot_index]
        .set(jnp.arange(row_count * top_count, dtype=jnp.int32) // top_count)
    )
    padded = jnp.concatenate([normed, jnp.zeros((1, width), jnp.bfloat16)], axis=0)
    outgoing = padded[owners].reshape(expert_count, capacity, width)
    gate_mat = w_gate[0]
    up_mat = w_up[0]
    down_mat = w_down[0]
    slice_width = width // tp_size
    own_columns = lax.dynamic_slice_in_dim(
        outgoing, lax.axis_index("tp") * slice_width, slice_width, 2
    )
    arrived = lax.all_to_all(own_columns, "ep", split_axis=0, concat_axis=0, tiled=True)
    piece = lax.all_gather(arrived, "tp", axis=2, tiled=True)
    gate = jnp.einsum("scd,df->scf", piece, gate_mat, preferred_element_type=jnp.float32)
    upward = jnp.einsum("scd,df->scf", piece, up_mat, preferred_element_type=jnp.float32)
    hidden = (jax.nn.silu(gate) * upward).astype(jnp.bfloat16)
    flat_hidden = hidden.reshape(-1, hidden.shape[2])
    summed = lax.psum_scatter(
        jnp.einsum("fd,sf->ds", down_mat, flat_hidden, preferred_element_type=jnp.float32).astype(
            jnp.bfloat16
        ),
        "tp",
        scatter_dimension=0,
        tiled=True,
    )
    back = lax.all_to_all(summed, "ep", split_axis=1, concat_axis=1, tiled=True)
    picked = (
        jnp.take(back, slot_index, axis=1).astype(jnp.float32).reshape(-1, row_count, top_count)
    )
    combined = jnp.einsum("drk,rk->rd", picked, route_weights)
    return combined.astype(jnp.bfloat16)


def experts(tokens, route_ids, route_weights, moe_gain, w_gate, w_up, w_down):
    row_count = tokens.shape[0]
    ep_size = lax.axis_size("ep")
    tp_size = lax.axis_size("tp")
    expert_count = w_gate.shape[0] * ep_size
    capacity = 2 * row_count * route_ids.shape[1] // expert_count
    whole = (
        capacity >= row_count
        and w_gate.shape[0] == 1
        and power_of_two(ep_size)
        and power_of_two(tp_size)
        and tp_size > 1
        and row_count % (16 * tp_size) == 0
        and w_gate.shape[2] % 128 == 0
        and tokens.shape[1] % (128 * tp_size) == 0
    )
    chosen = experts_whole if whole else experts_slots
    return chosen(tokens, route_ids, route_weights, moe_gain, w_gate, w_up, w_down)


def on_device(
    queries,
    keys,
    values,
    lambdas,
    head_gain,
    tokens,
    route_ids,
    route_weights,
    moe_gain,
    w_gate,
    w_up,
    w_down,
):
    heads_out = attend(queries, keys, values, lambdas, head_gain)
    expert_out = experts(tokens, route_ids, route_weights, moe_gain, w_gate, w_up, w_down)
    return (heads_out, expert_out)


def solution(mesh):
    in_specs = (
        P(("grp", "ep"), "tp"),
        P(("grp", "ep"), "tp"),
        P(("grp", "ep"), "tp"),
        P("tp"),
        P(),
        P(("grp", "ep"), None),
        P(("grp", "ep"), None),
        P(("grp", "ep"), None),
        P(),
        P("ep", None, "tp"),
        P("ep", None, "tp"),
        P("ep", "tp", None),
    )
    out_specs = (P(("grp", "ep"), "tp"), P(("grp", "ep"), "tp"))
    return jax.shard_map(
        on_device, mesh=mesh, in_specs=in_specs, out_specs=out_specs, check_vma=False
    )
```

```python
import math

import jax
import jax.numpy as jnp
from jax import lax
from jax.experimental import pallas as pl
from jax.experimental.pallas import tpu as pltpu
from jax.sharding import PartitionSpec as P


PREPARE_GRANT = 54 << 20
LOAD_GRANT = 46 << 20


def swap(value, axis, step):
    size = lax.axis_size(axis)
    return lax.ppermute(value, axis, [(i, i ^ step) for i in range(size)])


def halving_steps(size):
    steps = []
    step = size // 2
    while step >= 1:
        steps.append(step)
        step //= 2
    return steps


def power_of_two(size):
    return size & (size - 1) == 0


def attend(queries, keys, values, lambdas, head_gain):
    row_count = queries.shape[0]
    head_count = lambdas.shape[0]
    head_dim = queries.shape[1] // (2 * head_count)
    value_dim = values.shape[1] // head_count
    query_parts = queries.reshape(row_count, head_count, 2, head_dim)
    score_scale = head_dim ** (-0.5)
    running = jnp.full((head_count, 2, row_count), -1e30, jnp.float32)
    key_piece = lax.all_gather(keys, "ep", axis=0, tiled=True)
    value_piece = lax.all_gather(values, "ep", axis=0, tiled=True)
    count = key_piece.shape[0]
    key_parts = key_piece.reshape(count, head_count, 2, head_dim)
    value_parts = value_piece.reshape(count, head_count, value_dim)
    scores = (
        jnp.einsum("qhcd,khcd->hcqk", query_parts, key_parts, preferred_element_type=jnp.float32)
        * score_scale
    )
    newest = jnp.maximum(running, jnp.max(scores, axis=-1))
    weights_now = jnp.exp(scores - newest[..., None])
    totals = jnp.sum(weights_now, axis=-1)
    sums = jnp.einsum(
        "hcqk,khe->hcqe",
        weights_now.astype(jnp.bfloat16),
        value_parts,
        preferred_element_type=jnp.float32,
    )
    running, totals, sums = (newest, totals, sums)
    means = sums / totals[..., None]
    mixed = means[:, 0] - lambdas[:, None, None] * means[:, 1]
    scaled = mixed * lax.rsqrt(jnp.mean(mixed * mixed, axis=-1, keepdims=True) + 1e-06) * head_gain
    return (
        jnp.transpose(scaled, (1, 0, 2))
        .reshape(row_count, head_count * value_dim)
        .astype(jnp.bfloat16)
    )


def normalize(tokens, moe_gain):
    token_float = tokens.astype(jnp.float32)
    return (
        token_float
        * lax.rsqrt(jnp.mean(token_float * token_float, axis=1, keepdims=True) + 1e-06)
        * moe_gain
    ).astype(jnp.bfloat16)


def rms_rows(token_block, gain_row):
    token_float = token_block.astype(jnp.float32)
    scale = lax.rsqrt(jnp.mean(token_float * token_float, axis=1, keepdims=True) + 1e-06)
    return (token_float * scale * gain_row).astype(jnp.bfloat16)


def call(kernel, inputs, spaces, out_shapes, scratch, flops, grant):
    moved = sum(x.size * x.dtype.itemsize for x in inputs)
    moved += sum(math.prod(o.shape) * o.dtype.itemsize for o in out_shapes)
    return kernel_call(kernel, inputs, spaces, out_shapes, scratch, flops, moved, grant)


def kernel_call(kernel, inputs, spaces, out_shapes, scratch, flops, moved, grant):
    return pl.pallas_call(
        kernel,
        out_shape=out_shapes,
        in_specs=[pl.BlockSpec(memory_space=s) for s in spaces],
        out_specs=[pl.BlockSpec(memory_space=pltpu.VMEM)] * len(out_shapes),
        scratch_shapes=scratch,
        cost_estimate=pl.CostEstimate(flops=flops, bytes_accessed=moved, transcendentals=0),
        compiler_params=pltpu.CompilerParams(vmem_limit_bytes=grant),
    )(*inputs)


def reversed_bits(index, steps):
    part = jnp.zeros((), jnp.int32)
    for place, step in enumerate(steps):
        part = part + jnp.where(index & step != 0, 1 << place, 0)
    return part


def started(pairs, sems):
    copies = [
        pltpu.make_async_copy(source, target, sems.at[number])
        for number, (source, target) in enumerate(pairs)
    ]
    for copy in copies:
        copy.start()
    return copies


def prepare(tokens, moe_gain, keys, values, route_ids, route_weights):
    row_count, width = tokens.shape
    top_count = route_ids.shape[1]
    ep_size = lax.axis_size("ep")
    tp_size = lax.axis_size("tp")
    steps = halving_steps(tp_size)[:-1]
    piece_rows = row_count // tp_size
    half = row_count // 2
    key_width = keys.shape[1]
    lines = -(-ep_size // 128) * 128

    def kernel(token_ref, gain_ref, key_ref, value_ref, id_ref, scale_ref, *refs):
        piece_ref, half_ref, both_ref, weight_ref, rows, gains, ids, scales, table, sems = refs
        tp_index, ep_index = lax.axis_index("tp"), lax.axis_index("ep")
        at = pl.multiple_of((tp_index & 1) * half, half)
        copies = started(
            [
                (token_ref.at[pl.ds(at, half), :], rows),
                (gain_ref, gains),
                (id_ref, ids),
                (scale_ref, scales),
                (key_ref, both_ref.at[:, :key_width]),
                (value_ref, both_ref.at[:, key_width:]),
            ],
            sems,
        )
        for copy in copies[2:4]:
            copy.wait()
        table[...] = jnp.zeros_like(table)
        for step in range(ep_size):
            expert = ep_index ^ step
            line = jnp.zeros((1, row_count), jnp.float32)
            for choice in range(top_count):
                named = ids[choice : choice + 1, :] == expert
                line += jnp.where(named, scales[choice : choice + 1, :], 0.0)
            table[step : step + 1, :] = line
        weight_ref[...] = table[...].T
        for copy in copies[:2]:
            copy.wait()
        half_ref[...] = rms_rows(rows[...], gains[...].reshape(1, width))
        own = pl.multiple_of(reversed_bits(tp_index, steps) * piece_rows, piece_rows)
        piece_ref[...] = half_ref[pl.ds(own, piece_rows), :]
        for copy in copies[4:]:
            copy.wait()

    return call(
        kernel,
        (tokens, moe_gain, keys, values, route_ids.T, route_weights.T),
        (pltpu.HBM,) * 6,
        [
            jax.ShapeDtypeStruct((piece_rows, width), jnp.bfloat16),
            jax.ShapeDtypeStruct((half, width), jnp.bfloat16),
            jax.ShapeDtypeStruct((keys.shape[0], key_width + values.shape[1]), jnp.bfloat16),
            jax.ShapeDtypeStruct((row_count, lines), jnp.float32),
        ],
        [
            pltpu.VMEM((half, width), jnp.bfloat16),
            pltpu.VMEM((width,), jnp.float32),
            pltpu.VMEM((top_count, row_count), jnp.int32),
            pltpu.VMEM((top_count, row_count), jnp.float32),
            pltpu.VMEM((lines, row_count), jnp.float32),
            pltpu.SemaphoreType.DMA((6,)),
        ],
        8 * half * width,
        PREPARE_GRANT,
    )


def load(mats):
    def kernel(*refs):
        sources, targets, sems = refs[: len(mats)], refs[len(mats) : -1], refs[-1]
        for copy in started(list(zip(sources, targets)), sems):
            copy.wait()

    return call(
        kernel,
        tuple(mats),
        (pltpu.HBM,) * len(mats),
        [jax.ShapeDtypeStruct(m.shape, m.dtype) for m in mats],
        [pltpu.SemaphoreType.DMA((len(mats),))],
        1,
        LOAD_GRANT,
    )


def expert_kernel(pieces, mats):
    width, units = mats[0][0].shape
    tp_size = lax.axis_size("tp")
    steps = halving_steps(tp_size)[:-1]
    block_count = tp_size // 2
    block = width // block_count
    part_rows = pieces[0].shape[0]
    row_count = part_rows * len(pieces)
    half = block_count // 2
    chunk = math.gcd(units, 256)
    span = math.gcd(block, 384)

    def kernel(*refs):
        tp_index = lax.axis_index("tp")
        piece_refs, rest = refs[: len(pieces)], refs[len(pieces) :]
        mat_refs, (send_ref, keep_ref, rows, hidden) = rest[:-4], rest[-4:]
        sets = [mat_refs[i : i + 3] for i in range(0, len(mat_refs), 3)]
        if len(pieces) == 1:
            rows[...] = piece_refs[0][...]
        else:
            flips = [0]
            for step in steps:
                flips = flips + [f ^ step for f in flips]
            for flip, ref in zip(flips, piece_refs):
                at = reversed_bits(tp_index ^ flip, steps) * part_rows
                at = pl.multiple_of(at, part_rows)
                rows[pl.ds(at, part_rows), :] = ref[...]
        for number, (gate_ref, up_ref, _) in enumerate(sets):
            for step in range(units // chunk):
                columns = pl.ds(step * chunk, chunk)
                gate = jnp.dot(rows[...], gate_ref[:, columns], preferred_element_type=jnp.float32)
                upward = jnp.dot(rows[...], up_ref[:, columns], preferred_element_type=jnp.float32)
                result = gate / (1.0 + jnp.exp(-gate)) * upward
                hidden[:, pl.ds(number * units + step * chunk, chunk)] = result.astype(jnp.bfloat16)
        for index in range(block_count):
            target = send_ref if index < half else keep_ref
            owner = tp_index >> 1
            for bit, step in enumerate(steps):
                if not (index >> bit) & 1:
                    owner = owner ^ (step >> 1)
            for step in range(block // span):
                at = pl.multiple_of(owner * block + step * span, span)
                out = jnp.zeros((row_count, span), jnp.float32)
                for number, (_, _, down_ref) in enumerate(sets):
                    out += jnp.dot(
                        hidden[:, number * units : (number + 1) * units],
                        down_ref[:, pl.ds(at, span)],
                        preferred_element_type=jnp.float32,
                    )
                start = (index % half) * block + step * span
                target[:, start : start + span] = out.astype(jnp.bfloat16)

    flat_mats = tuple(m for group in mats for m in group)
    inputs = (*pieces, *flat_mats)
    spaces = (pltpu.VMEM,) * len(inputs)
    shape = jax.ShapeDtypeStruct((row_count, half * block), jnp.bfloat16)
    return call(
        kernel,
        inputs,
        spaces,
        [shape, shape],
        [
            pltpu.VMEM((row_count, width), jnp.bfloat16),
            pltpu.VMEM((row_count, units * len(mats)), jnp.bfloat16),
        ],
        6 * row_count * width * units * len(mats),
        10 << 20,
    )


def add_halves(kept, came):
    row_count, columns = kept.shape
    half = columns // 2

    def kernel(kept_ref, came_ref, send_ref, keep_ref):
        for ref, at in ((send_ref, 0), (keep_ref, half)):
            one = kept_ref[:, at : at + half].astype(jnp.float32)
            two = came_ref[:, at : at + half].astype(jnp.float32)
            ref[...] = (one + two).astype(jnp.bfloat16)

    shape = jax.ShapeDtypeStruct((row_count, half), jnp.bfloat16)
    return call(
        kernel, (kept, came), (pltpu.VMEM,) * 2, [shape, shape], [], row_count * columns, 4 << 20
    )


def add_last(kept, came):
    def kernel(kept_ref, came_ref, out_ref):
        out_ref[...] = (
            kept_ref[...].astype(jnp.float32) + came_ref[...].astype(jnp.float32)
        ).astype(jnp.bfloat16)

    return call(
        kernel,
        (kept, came),
        (pltpu.VMEM,) * 2,
        [jax.ShapeDtypeStruct(kept.shape, jnp.bfloat16)],
        [],
        kept.size,
        4 << 20,
    )[0]


def weighted_sum(weights, own, results):
    row_count, columns = results[0].shape
    half = columns // 2

    def kernel(weight_ref, kept_ref, came_ref, *refs):
        result_refs, (send_ref, keep_ref) = refs[:-2], refs[-2:]
        core = lax.axis_index("tp") & 1
        first = pl.multiple_of(core * row_count, row_count)
        for ref, side in ((send_ref, 1 - core), (keep_ref, core)):
            at = pl.multiple_of(side * half, half)
            total = jnp.zeros((row_count, half), jnp.float32)
            for step in range(len(results) + 1):
                weight = weight_ref[pl.ds(first, row_count), step : step + 1]
                if step == 0:
                    result = kept_ref[:, pl.ds(at, half)].astype(jnp.float32)
                    result += came_ref[:, pl.ds(at, half)].astype(jnp.float32)
                else:
                    result = result_refs[step - 1][:, pl.ds(at, half)].astype(jnp.float32)
                total += jnp.where(weight != 0.0, result * weight, 0.0)
            ref[...] = total.astype(jnp.bfloat16)

    inputs = (weights, *own, *results)
    shape = jax.ShapeDtypeStruct((row_count, half), jnp.bfloat16)
    return call(
        kernel,
        inputs,
        (pltpu.VMEM,) * len(inputs),
        [shape, shape],
        [],
        8 * row_count * columns,
        8 << 20,
    )


def both_halves(kept, came):
    row_count, columns = kept.shape

    def kernel(kept_ref, came_ref, out_ref):
        core = lax.axis_index("tp") & 1
        mine = pl.multiple_of(core * row_count, row_count)
        other = pl.multiple_of((1 - core) * row_count, row_count)
        out_ref[pl.ds(mine, row_count), :] = kept_ref[...]
        out_ref[pl.ds(other, row_count), :] = came_ref[...]

    return call(
        kernel,
        (kept, came),
        (pltpu.VMEM,) * 2,
        [jax.ShapeDtypeStruct((2 * row_count, columns), jnp.bfloat16)],
        [],
        row_count * columns,
        4 << 20,
    )[0]


def attention(queries, keys, values, others, lambdas, head_gain):
    row_count, width = queries.shape
    head_count = lambdas.shape[0]
    pair = width // head_count
    head_dim = pair // 2
    value_dim = values.shape[1] // head_count
    count = row_count * (len(others) + 1)
    score_scale = head_dim ** (-0.5)

    def kernel(lambda_ref, gain_ref, query_ref, key_ref, value_ref, *refs):
        other_refs, (out_ref, all_keys, all_values) = refs[:-3], refs[-3:]
        all_keys[:row_count, :] = key_ref[...]
        all_values[:row_count, :] = value_ref[...]
        for index, ref in enumerate(other_refs):
            rows = slice((index + 1) * row_count, (index + 2) * row_count)
            all_keys[rows, :] = ref[:, :width]
            all_values[rows, :] = ref[:, width:]
        lane = lax.broadcasted_iota(jnp.int32, (row_count, pair), 1)
        for head in range(head_count):
            query = query_ref[:, head * pair : (head + 1) * pair]
            key = all_keys[:, head * pair : (head + 1) * pair]
            value = all_values[:, head * value_dim : (head + 1) * value_dim]
            means = []
            for part in range(2):
                here = (lane < head_dim) if part == 0 else (lane >= head_dim)
                masked = jnp.where(here, query, jnp.zeros_like(query))
                scores = (
                    lax.dot_general(
                        masked, key, (((1,), (1,)), ((), ())), preferred_element_type=jnp.float32
                    )
                    * score_scale
                )
                raised = jnp.exp(scores - jnp.max(scores, axis=1, keepdims=True))
                totals = jnp.sum(raised, axis=1, keepdims=True)
                sums = jnp.dot(
                    raised.astype(jnp.bfloat16), value, preferred_element_type=jnp.float32
                )
                means.append(sums / totals)
            mixed = means[0] - lambda_ref[head] * means[1]
            scale = lax.rsqrt(jnp.mean(mixed * mixed, axis=1, keepdims=True) + 1e-06)
            out_ref[:, head * value_dim : (head + 1) * value_dim] = (
                mixed * scale * gain_ref[...].reshape(1, value_dim)
            ).astype(jnp.bfloat16)

    inputs = (lambdas, head_gain, queries, keys, values, *others)
    return call(
        kernel,
        inputs,
        (pltpu.SMEM,) + (pltpu.VMEM,) * (len(inputs) - 1),
        [jax.ShapeDtypeStruct((row_count, head_count * value_dim), jnp.bfloat16)],
        [
            pltpu.VMEM((count, width), jnp.bfloat16),
            pltpu.VMEM((count, values.shape[1]), jnp.bfloat16),
        ],
        4 * row_count * count * (width + 2 * values.shape[1]),
        12 << 20,
    )[0]


def whole_rows(
    queries, keys, values, lambdas, head_gain, tokens, route_ids, route_weights, moe_gain, *mats
):
    ep_size = lax.axis_size("ep")
    tp_size = lax.axis_size("tp")
    steps = halving_steps(tp_size)[:-1]
    mine, own_rows, both, weights = prepare(
        tokens, moe_gain, keys, values, route_ids, route_weights
    )
    mats = [m[0] for m in mats]
    others_mats = [swap(m, "tp", 1) for m in mats]
    mats = (load(mats), others_mats)

    def gathered(piece):
        pieces = [piece]
        for place in range(1, ep_size):
            low = place & -place
            pieces.append(swap(pieces[place ^ low], "ep", low))
        return pieces[1:]

    arrivals = gathered(mine)
    others = gathered(both)

    def half_rows(piece):
        pieces = [piece]
        for step in steps:
            pieces = pieces + [swap(p, "tp", step) for p in pieces]
        return pieces

    def reduced(send, keep, last):
        for step in reversed(steps):
            came = swap(send, "tp", step)
            if step == steps[0]:
                return add_last(keep, came) if last else (keep, came)
            send, keep = add_halves(keep, came)

    own = expert_kernel([own_rows], mats)
    own = reduced(*own, False)
    results = []
    for step in range(1, ep_size):
        pieces = half_rows(arrivals[step - 1])
        done = expert_kernel(pieces, mats)
        done = reduced(*done, True)
        results.append(swap(done, "ep", step))
    heads_out = attention(queries, keys, values, others, lambdas, head_gain)
    send, keep = weighted_sum(weights, own, results)
    came = swap(send, "tp", 1)
    return heads_out, both_halves(keep, came)


def experts_slots(tokens, route_ids, route_weights, moe_gain, w_gate, w_up, w_down):
    row_count, width = tokens.shape
    top_count = route_ids.shape[1]
    ep_size = lax.axis_size("ep")
    tp_size = lax.axis_size("tp")
    expert_count = w_gate.shape[0] * ep_size
    capacity = 2 * row_count * top_count // expert_count
    normed = normalize(tokens, moe_gain)
    flat_ids = route_ids.reshape(-1)
    onehot = (flat_ids[:, None] == jnp.arange(expert_count, dtype=jnp.int32)[None, :]).astype(
        jnp.int32
    )
    earlier = jnp.cumsum(onehot, axis=0) - onehot
    position = jnp.sum(earlier * onehot, axis=1)
    slot_index = flat_ids * capacity + position
    owners = (
        jnp.full((expert_count * capacity,), row_count, jnp.int32)
        .at[slot_index]
        .set(jnp.arange(row_count * top_count, dtype=jnp.int32) // top_count)
    )
    padded = jnp.concatenate([normed, jnp.zeros((1, width), jnp.bfloat16)], axis=0)
    outgoing = padded[owners].reshape(expert_count, capacity, width)
    gate_mat = w_gate[0]
    up_mat = w_up[0]
    down_mat = w_down[0]
    slice_width = width // tp_size
    own_columns = lax.dynamic_slice_in_dim(
        outgoing, lax.axis_index("tp") * slice_width, slice_width, 2
    )
    arrived = lax.all_to_all(own_columns, "ep", split_axis=0, concat_axis=0, tiled=True)
    piece = lax.all_gather(arrived, "tp", axis=2, tiled=True)
    gate = jnp.einsum("scd,df->scf", piece, gate_mat, preferred_element_type=jnp.float32)
    upward = jnp.einsum("scd,df->scf", piece, up_mat, preferred_element_type=jnp.float32)
    hidden = (jax.nn.silu(gate) * upward).astype(jnp.bfloat16)
    flat_hidden = hidden.reshape(-1, hidden.shape[2])
    summed = lax.psum_scatter(
        jnp.einsum("fd,sf->ds", down_mat, flat_hidden, preferred_element_type=jnp.float32).astype(
            jnp.bfloat16
        ),
        "tp",
        scatter_dimension=0,
        tiled=True,
    )
    back = lax.all_to_all(summed, "ep", split_axis=1, concat_axis=1, tiled=True)
    picked = (
        jnp.take(back, slot_index, axis=1).astype(jnp.float32).reshape(-1, row_count, top_count)
    )
    combined = jnp.einsum("drk,rk->rd", picked, route_weights)
    return combined.astype(jnp.bfloat16)


def fits_whole(queries, keys, values, lambdas, tokens, route_ids, w_gate):
    row_count, width = tokens.shape
    ep_size = lax.axis_size("ep")
    tp_size = lax.axis_size("tp")
    expert_count = w_gate.shape[0] * ep_size
    capacity = 2 * row_count * route_ids.shape[1] // expert_count
    return (
        capacity >= row_count
        and w_gate.shape[0] == 1
        and power_of_two(ep_size)
        and power_of_two(tp_size)
        and tp_size >= 4
        and row_count % (16 * tp_size) == 0
        and w_gate.shape[2] % 128 == 0
        and width % (128 * tp_size) == 0
        and queries.shape[1] % (128 * lambdas.shape[0]) == 0
        and values.shape[1] % (128 * lambdas.shape[0]) == 0
        and keys.shape[0] % 128 == 0
    )


def on_device(
    queries,
    keys,
    values,
    lambdas,
    head_gain,
    tokens,
    route_ids,
    route_weights,
    moe_gain,
    w_gate,
    w_up,
    w_down,
):
    routed = (tokens, route_ids, route_weights, moe_gain, w_gate, w_up, w_down)
    if fits_whole(queries, keys, values, lambdas, tokens, route_ids, w_gate):
        return whole_rows(queries, keys, values, lambdas, head_gain, *routed)
    heads_out = attend(queries, keys, values, lambdas, head_gain)
    return (heads_out, experts_slots(*routed))


def solution(mesh):
    in_specs = (
        P(("grp", "ep"), "tp"),
        P(("grp", "ep"), "tp"),
        P(("grp", "ep"), "tp"),
        P("tp"),
        P(),
        P(("grp", "ep"), None),
        P(("grp", "ep"), None),
        P(("grp", "ep"), None),
        P(),
        P("ep", None, "tp"),
        P("ep", None, "tp"),
        P("ep", "tp", None),
    )
    out_specs = (P(("grp", "ep"), "tp"), P(("grp", "ep"), "tp"))
    return jax.shard_map(
        on_device, mesh=mesh, in_specs=in_specs, out_specs=out_specs, check_vma=False
    )
```

```python
import math

import jax
import jax.numpy as jnp
from jax import lax
from jax.experimental import pallas as pl
from jax.experimental.pallas import tpu as pltpu
from jax.sharding import PartitionSpec as P


PREPARE_GRANT = 54 << 20
REST_GRANT = 54 << 20
LOAD_GRANT = 46 << 20


def swap(value, axis, step):
    size = lax.axis_size(axis)
    return lax.ppermute(value, axis, [(i, i ^ step) for i in range(size)])


def halving_steps(size):
    steps = []
    step = size // 2
    while step >= 1:
        steps.append(step)
        step //= 2
    return steps


def power_of_two(size):
    return size & (size - 1) == 0


def attend(queries, keys, values, lambdas, head_gain):
    row_count = queries.shape[0]
    head_count = lambdas.shape[0]
    head_dim = queries.shape[1] // (2 * head_count)
    value_dim = values.shape[1] // head_count
    query_parts = queries.reshape(row_count, head_count, 2, head_dim)
    score_scale = head_dim ** (-0.5)
    running = jnp.full((head_count, 2, row_count), -1e30, jnp.float32)
    key_piece = lax.all_gather(keys, "ep", axis=0, tiled=True)
    value_piece = lax.all_gather(values, "ep", axis=0, tiled=True)
    count = key_piece.shape[0]
    key_parts = key_piece.reshape(count, head_count, 2, head_dim)
    value_parts = value_piece.reshape(count, head_count, value_dim)
    scores = (
        jnp.einsum("qhcd,khcd->hcqk", query_parts, key_parts, preferred_element_type=jnp.float32)
        * score_scale
    )
    newest = jnp.maximum(running, jnp.max(scores, axis=-1))
    weights_now = jnp.exp(scores - newest[..., None])
    totals = jnp.sum(weights_now, axis=-1)
    sums = jnp.einsum(
        "hcqk,khe->hcqe",
        weights_now.astype(jnp.bfloat16),
        value_parts,
        preferred_element_type=jnp.float32,
    )
    running, totals, sums = (newest, totals, sums)
    means = sums / totals[..., None]
    mixed = means[:, 0] - lambdas[:, None, None] * means[:, 1]
    scaled = mixed * lax.rsqrt(jnp.mean(mixed * mixed, axis=-1, keepdims=True) + 1e-06) * head_gain
    return (
        jnp.transpose(scaled, (1, 0, 2))
        .reshape(row_count, head_count * value_dim)
        .astype(jnp.bfloat16)
    )


def normalize(tokens, moe_gain):
    token_float = tokens.astype(jnp.float32)
    return (
        token_float
        * lax.rsqrt(jnp.mean(token_float * token_float, axis=1, keepdims=True) + 1e-06)
        * moe_gain
    ).astype(jnp.bfloat16)


def rms_rows(token_block, gain_row):
    token_float = token_block.astype(jnp.float32)
    scale = lax.rsqrt(jnp.mean(token_float * token_float, axis=1, keepdims=True) + 1e-06)
    return (token_float * scale * gain_row).astype(jnp.bfloat16)


def call(kernel, inputs, spaces, out_shapes, scratch, flops, grant):
    moved = sum(x.size * x.dtype.itemsize for x in inputs)
    moved += sum(math.prod(o.shape) * o.dtype.itemsize for o in out_shapes)
    return kernel_call(kernel, inputs, spaces, out_shapes, scratch, flops, moved, grant)


def kernel_call(kernel, inputs, spaces, out_shapes, scratch, flops, moved, grant):
    return pl.pallas_call(
        kernel,
        out_shape=out_shapes,
        in_specs=[pl.BlockSpec(memory_space=s) for s in spaces],
        out_specs=[pl.BlockSpec(memory_space=pltpu.VMEM)] * len(out_shapes),
        scratch_shapes=scratch,
        cost_estimate=pl.CostEstimate(flops=flops, bytes_accessed=moved, transcendentals=0),
        compiler_params=pltpu.CompilerParams(vmem_limit_bytes=grant),
    )(*inputs)


def reversed_bits(index, steps):
    part = jnp.zeros((), jnp.int32)
    for place, step in enumerate(steps):
        part = part + jnp.where(index & step != 0, 1 << place, 0)
    return part


def started(pairs, sems):
    copies = [
        pltpu.make_async_copy(source, target, sems.at[number])
        for number, (source, target) in enumerate(pairs)
    ]
    for copy in copies:
        copy.start()
    return copies


def part_flips(steps):
    flips = [0]
    for step in steps:
        flips = flips + [f ^ step for f in flips]
    return flips


def prepare(tokens, moe_gain):
    row_count, width = tokens.shape
    tp_size = lax.axis_size("tp")
    steps = halving_steps(tp_size)[:-1]
    piece_rows = row_count // tp_size

    def kernel(token_ref, gain_ref, piece_ref, rows, gains, sems):
        tp_index = lax.axis_index("tp")
        part = (tp_index & 1) * (tp_size // 2) + reversed_bits(tp_index, steps)
        at = pl.multiple_of(part * piece_rows, piece_rows)
        pairs = [(token_ref.at[pl.ds(at, piece_rows), :], rows), (gain_ref, gains)]
        for copy in started(pairs, sems):
            copy.wait()
        piece_ref[...] = rms_rows(rows[...], gains[...].reshape(1, width))

    return call(
        kernel,
        (tokens, moe_gain),
        (pltpu.HBM,) * 2,
        [jax.ShapeDtypeStruct((piece_rows, width), jnp.bfloat16)],
        [
            pltpu.VMEM((piece_rows, width), jnp.bfloat16),
            pltpu.VMEM((width,), jnp.float32),
            pltpu.SemaphoreType.DMA((2,)),
        ],
        8 * piece_rows * width,
        PREPARE_GRANT,
    )[0]


def rest(tokens, moe_gain, keys, values, route_ids, route_weights):
    row_count, width = tokens.shape
    top_count = route_ids.shape[1]
    ep_size = lax.axis_size("ep")
    half = row_count // 2
    key_width = keys.shape[1]
    lines = -(-ep_size // 128) * 128

    def kernel(token_ref, gain_ref, key_ref, value_ref, id_ref, scale_ref, *refs):
        half_ref, both_ref, weight_ref = refs[:-6]
        rows, gains, ids, scales, table, sems = refs[-6:]
        ep_index = lax.axis_index("ep")
        at = pl.multiple_of((lax.axis_index("tp") & 1) * half, half)
        copies = started(
            [
                (token_ref.at[pl.ds(at, half), :], rows),
                (gain_ref, gains),
                (id_ref, ids),
                (scale_ref, scales),
                (key_ref, both_ref.at[:, :key_width]),
                (value_ref, both_ref.at[:, key_width:]),
            ],
            sems,
        )
        for copy in copies[2:4]:
            copy.wait()
        table[...] = jnp.zeros_like(table)
        for step in range(ep_size):
            expert = ep_index ^ step
            line = jnp.zeros((1, row_count), jnp.float32)
            for choice in range(top_count):
                named = ids[choice : choice + 1, :] == expert
                line += jnp.where(named, scales[choice : choice + 1, :], 0.0)
            table[step : step + 1, :] = line
        weight_ref[...] = table[...].T
        for copy in copies[:2]:
            copy.wait()
        half_ref[...] = rms_rows(rows[...], gains[...].reshape(1, width))
        for copy in copies[4:]:
            copy.wait()

    return call(
        kernel,
        (tokens, moe_gain, keys, values, route_ids.T, route_weights.T),
        (pltpu.HBM,) * 6,
        [
            jax.ShapeDtypeStruct((half, width), jnp.bfloat16),
            jax.ShapeDtypeStruct((keys.shape[0], key_width + values.shape[1]), jnp.bfloat16),
            jax.ShapeDtypeStruct((row_count, lines), jnp.float32),
        ],
        [
            pltpu.VMEM((half, width), jnp.bfloat16),
            pltpu.VMEM((width,), jnp.float32),
            pltpu.VMEM((top_count, row_count), jnp.int32),
            pltpu.VMEM((top_count, row_count), jnp.float32),
            pltpu.VMEM((lines, row_count), jnp.float32),
            pltpu.SemaphoreType.DMA((6,)),
        ],
        8 * half * width,
        REST_GRANT,
    )


def load(mats):
    def kernel(*refs):
        sources, targets, sems = refs[: len(mats)], refs[len(mats) : -1], refs[-1]
        for copy in started(list(zip(sources, targets)), sems):
            copy.wait()

    return call(
        kernel,
        tuple(mats),
        (pltpu.HBM,) * len(mats),
        [jax.ShapeDtypeStruct(m.shape, m.dtype) for m in mats],
        [pltpu.SemaphoreType.DMA((len(mats),))],
        1,
        LOAD_GRANT,
    )


def expert_kernel(pieces, mats):
    width, units = mats[0][0].shape
    tp_size = lax.axis_size("tp")
    steps = halving_steps(tp_size)[:-1]
    block_count = tp_size // 2
    block = width // block_count
    part_rows = pieces[0].shape[0]
    row_count = part_rows * len(pieces)
    half = block_count // 2
    chunk = math.gcd(units, 256)
    span = math.gcd(block, 384)

    def kernel(*refs):
        tp_index = lax.axis_index("tp")
        piece_refs, rest = refs[: len(pieces)], refs[len(pieces) :]
        mat_refs, (send_ref, keep_ref, rows, hidden) = rest[:-4], rest[-4:]
        sets = [mat_refs[i : i + 3] for i in range(0, len(mat_refs), 3)]
        if len(pieces) == 1:
            rows[...] = piece_refs[0][...]
        else:
            for flip, ref in zip(part_flips(steps), piece_refs):
                at = reversed_bits(tp_index ^ flip, steps) * part_rows
                at = pl.multiple_of(at, part_rows)
                rows[pl.ds(at, part_rows), :] = ref[...]
        for number, (gate_ref, up_ref, _) in enumerate(sets):
            for step in range(units // chunk):
                columns = pl.ds(step * chunk, chunk)
                gate = jnp.dot(rows[...], gate_ref[:, columns], preferred_element_type=jnp.float32)
                upward = jnp.dot(rows[...], up_ref[:, columns], preferred_element_type=jnp.float32)
                result = gate / (1.0 + jnp.exp(-gate)) * upward
                hidden[:, pl.ds(number * units + step * chunk, chunk)] = result.astype(jnp.bfloat16)
        for index in range(block_count):
            target = send_ref if index < half else keep_ref
            owner = tp_index >> 1
            for bit, step in enumerate(steps):
                if not (index >> bit) & 1:
                    owner = owner ^ (step >> 1)
            for step in range(block // span):
                at = pl.multiple_of(owner * block + step * span, span)
                out = jnp.zeros((row_count, span), jnp.float32)
                for number, (_, _, down_ref) in enumerate(sets):
                    out += jnp.dot(
                        hidden[:, number * units : (number + 1) * units],
                        down_ref[:, pl.ds(at, span)],
                        preferred_element_type=jnp.float32,
                    )
                start = (index % half) * block + step * span
                target[:, start : start + span] = out.astype(jnp.bfloat16)

    flat_mats = tuple(m for group in mats for m in group)
    inputs = (*pieces, *flat_mats)
    spaces = (pltpu.VMEM,) * len(inputs)
    shape = jax.ShapeDtypeStruct((row_count, half * block), jnp.bfloat16)
    return call(
        kernel,
        inputs,
        spaces,
        [shape, shape],
        [
            pltpu.VMEM((row_count, width), jnp.bfloat16),
            pltpu.VMEM((row_count, units * len(mats)), jnp.bfloat16),
        ],
        6 * row_count * width * units * len(mats),
        10 << 20,
    )


def add_halves(kept, came):
    row_count, columns = kept.shape
    half = columns // 2

    def kernel(kept_ref, came_ref, send_ref, keep_ref):
        for ref, at in ((send_ref, 0), (keep_ref, half)):
            one = kept_ref[:, at : at + half].astype(jnp.float32)
            two = came_ref[:, at : at + half].astype(jnp.float32)
            ref[...] = (one + two).astype(jnp.bfloat16)

    shape = jax.ShapeDtypeStruct((row_count, half), jnp.bfloat16)
    return call(
        kernel, (kept, came), (pltpu.VMEM,) * 2, [shape, shape], [], row_count * columns, 4 << 20
    )


def add_last(kept, came):
    def kernel(kept_ref, came_ref, out_ref):
        out_ref[...] = (
            kept_ref[...].astype(jnp.float32) + came_ref[...].astype(jnp.float32)
        ).astype(jnp.bfloat16)

    return call(
        kernel,
        (kept, came),
        (pltpu.VMEM,) * 2,
        [jax.ShapeDtypeStruct(kept.shape, jnp.bfloat16)],
        [],
        kept.size,
        4 << 20,
    )[0]


def terms(weight_ref, rows, numbers_and_results):
    total = None
    for number, result in numbers_and_results:
        weight = weight_ref[rows, number : number + 1]
        term = jnp.where(weight != 0.0, result * weight, 0.0)
        total = term if total is None else total + term
    return total


def early_sum(weights, own, results):
    row_count, columns = own[0].shape
    half = columns // 2

    def kernel(weight_ref, kept_ref, came_ref, *refs):
        result_refs, (send_ref, keep_ref) = refs[:-2], refs[-2:]
        core = lax.axis_index("tp") & 1
        rows = pl.ds(pl.multiple_of(core * row_count, row_count), row_count)
        for ref, side in ((send_ref, 1 - core), (keep_ref, core)):
            at = pl.ds(pl.multiple_of(side * half, half), half)
            own_result = kept_ref[:, at].astype(jnp.float32) + came_ref[:, at].astype(jnp.float32)
            numbered = [(0, own_result)]
            for number, result_ref in zip(results, result_refs):
                numbered.append((number, result_ref[:, at].astype(jnp.float32)))
            ref[...] = terms(weight_ref, rows, numbered)

    inputs = (weights, *own, *results.values())
    shape = jax.ShapeDtypeStruct((row_count, half), jnp.float32)
    return call(
        kernel,
        inputs,
        (pltpu.VMEM,) * len(inputs),
        [shape, shape],
        [],
        8 * row_count * columns,
        8 << 20,
    )


def add_columns(kept, came):
    row_count, columns = kept.shape
    half = columns // 2

    def kernel(kept_ref, came_ref, same_ref, cross_ref):
        core = lax.axis_index("tp") & 1
        for ref, side in ((same_ref, core), (cross_ref, 1 - core)):
            at = pl.ds(pl.multiple_of(side * half, half), half)
            one = kept_ref[:, at].astype(jnp.float32)
            ref[...] = (one + came_ref[:, at].astype(jnp.float32)).astype(jnp.bfloat16)

    shape = jax.ShapeDtypeStruct((row_count, half), jnp.bfloat16)
    return call(
        kernel, (kept, came), (pltpu.VMEM,) * 2, [shape, shape], [], row_count * columns, 4 << 20
    )


def final_sum(weights, number, kept, came, same, cross):
    row_count, columns = kept.shape

    def kernel(weight_ref, kept_ref, came_ref, same_ref, cross_ref, out_ref):
        core = lax.axis_index("tp") & 1
        for side, early_ref, result_ref in ((core, kept_ref, same_ref), (1 - core, came_ref, cross_ref)):
            rows = pl.ds(pl.multiple_of(side * row_count, row_count), row_count)
            last = terms(weight_ref, rows, [(number, result_ref[...].astype(jnp.float32))])
            out_ref[rows, :] = (early_ref[...] + last).astype(jnp.bfloat16)

    return call(
        kernel,
        (weights, kept, came, same, cross),
        (pltpu.VMEM,) * 5,
        [jax.ShapeDtypeStruct((2 * row_count, columns), jnp.bfloat16)],
        [],
        8 * row_count * columns,
        8 << 20,
    )[0]


def attention(queries, keys, values, others, lambdas, head_gain):
    row_count, width = queries.shape
    head_count = lambdas.shape[0]
    pair = width // head_count
    head_dim = pair // 2
    value_dim = values.shape[1] // head_count
    count = row_count * (len(others) + 1)
    score_scale = head_dim ** (-0.5)

    def kernel(lambda_ref, gain_ref, query_ref, key_ref, value_ref, *refs):
        other_refs, (out_ref, all_keys, all_values) = refs[:-3], refs[-3:]
        all_keys[:row_count, :] = key_ref[...]
        all_values[:row_count, :] = value_ref[...]
        for index, ref in enumerate(other_refs):
            rows = slice((index + 1) * row_count, (index + 2) * row_count)
            all_keys[rows, :] = ref[:, :width]
            all_values[rows, :] = ref[:, width:]
        lane = lax.broadcasted_iota(jnp.int32, (row_count, pair), 1)
        for head in range(head_count):
            query = query_ref[:, head * pair : (head + 1) * pair]
            key = all_keys[:, head * pair : (head + 1) * pair]
            value = all_values[:, head * value_dim : (head + 1) * value_dim]
            means = []
            for part in range(2):
                here = (lane < head_dim) if part == 0 else (lane >= head_dim)
                masked = jnp.where(here, query, jnp.zeros_like(query))
                scores = (
                    lax.dot_general(
                        masked, key, (((1,), (1,)), ((), ())), preferred_element_type=jnp.float32
                    )
                    * score_scale
                )
                raised = jnp.exp(scores - jnp.max(scores, axis=1, keepdims=True))
                totals = jnp.sum(raised, axis=1, keepdims=True)
                sums = jnp.dot(
                    raised.astype(jnp.bfloat16), value, preferred_element_type=jnp.float32
                )
                means.append(sums / totals)
            mixed = means[0] - lambda_ref[head] * means[1]
            scale = lax.rsqrt(jnp.mean(mixed * mixed, axis=1, keepdims=True) + 1e-06)
            out_ref[:, head * value_dim : (head + 1) * value_dim] = (
                mixed * scale * gain_ref[...].reshape(1, value_dim)
            ).astype(jnp.bfloat16)

    inputs = (lambdas, head_gain, queries, keys, values, *others)
    return call(
        kernel,
        inputs,
        (pltpu.SMEM,) + (pltpu.VMEM,) * (len(inputs) - 1),
        [jax.ShapeDtypeStruct((row_count, head_count * value_dim), jnp.bfloat16)],
        [
            pltpu.VMEM((count, width), jnp.bfloat16),
            pltpu.VMEM((count, values.shape[1]), jnp.bfloat16),
        ],
        4 * row_count * count * (width + 2 * values.shape[1]),
        12 << 20,
    )[0]


def whole_rows(
    queries, keys, values, lambdas, head_gain, tokens, route_ids, route_weights, moe_gain, *mats
):
    ep_size = lax.axis_size("ep")
    tp_size = lax.axis_size("tp")
    steps = halving_steps(tp_size)[:-1]
    mine = prepare(tokens, moe_gain)
    own_rows, both, weights = rest(
        tokens, moe_gain, keys, values, route_ids, route_weights
    )
    mats = [m[0] for m in mats]
    others_mats = [swap(m, "tp", 1) for m in mats]
    mats = (load(mats), others_mats)

    def gathered(piece):
        pieces = [piece]
        for place in range(1, ep_size):
            low = place & -place
            pieces.append(swap(pieces[place ^ low], "ep", low))
        return pieces[1:]

    arrivals = gathered(mine)
    others = gathered(both)

    def half_rows(piece):
        pieces = [piece]
        for step in steps:
            pieces = pieces + [swap(p, "tp", step) for p in pieces]
        return pieces

    def reduced(send, keep, last):
        for step in reversed(steps):
            came = swap(send, "tp", step)
            if step == steps[0]:
                return add_last(keep, came) if last else (keep, came)
            send, keep = add_halves(keep, came)

    own = expert_kernel([own_rows], mats)
    own = reduced(*own, False)
    results, last = {}, 1
    for step in range(1, ep_size):
        pieces = half_rows(arrivals[step - 1])
        done = expert_kernel(pieces, mats)
        done = reduced(*done, step != last)
        if step == last:
            same, cross = add_columns(*done)
            same = swap(same, "ep", step)
            cross = swap(cross, ("ep", "tp"), step * tp_size + 1)
        else:
            results[step] = swap(done, "ep", step)
    heads_out = attention(queries, keys, values, others, lambdas, head_gain)
    send, keep = early_sum(weights, own, results)
    came = swap(send, "tp", 1)
    return heads_out, final_sum(weights, last, keep, came, same, cross)


def experts_slots(tokens, route_ids, route_weights, moe_gain, w_gate, w_up, w_down):
    row_count, width = tokens.shape
    top_count = route_ids.shape[1]
    ep_size = lax.axis_size("ep")
    tp_size = lax.axis_size("tp")
    expert_count = w_gate.shape[0] * ep_size
    capacity = 2 * row_count * top_count // expert_count
    normed = normalize(tokens, moe_gain)
    flat_ids = route_ids.reshape(-1)
    onehot = (flat_ids[:, None] == jnp.arange(expert_count, dtype=jnp.int32)[None, :]).astype(
        jnp.int32
    )
    earlier = jnp.cumsum(onehot, axis=0) - onehot
    position = jnp.sum(earlier * onehot, axis=1)
    slot_index = flat_ids * capacity + position
    owners = (
        jnp.full((expert_count * capacity,), row_count, jnp.int32)
        .at[slot_index]
        .set(jnp.arange(row_count * top_count, dtype=jnp.int32) // top_count)
    )
    padded = jnp.concatenate([normed, jnp.zeros((1, width), jnp.bfloat16)], axis=0)
    outgoing = padded[owners].reshape(expert_count, capacity, width)
    gate_mat = w_gate[0]
    up_mat = w_up[0]
    down_mat = w_down[0]
    slice_width = width // tp_size
    own_columns = lax.dynamic_slice_in_dim(
        outgoing, lax.axis_index("tp") * slice_width, slice_width, 2
    )
    arrived = lax.all_to_all(own_columns, "ep", split_axis=0, concat_axis=0, tiled=True)
    piece = lax.all_gather(arrived, "tp", axis=2, tiled=True)
    gate = jnp.einsum("scd,df->scf", piece, gate_mat, preferred_element_type=jnp.float32)
    upward = jnp.einsum("scd,df->scf", piece, up_mat, preferred_element_type=jnp.float32)
    hidden = (jax.nn.silu(gate) * upward).astype(jnp.bfloat16)
    flat_hidden = hidden.reshape(-1, hidden.shape[2])
    summed = lax.psum_scatter(
        jnp.einsum("fd,sf->ds", down_mat, flat_hidden, preferred_element_type=jnp.float32).astype(
            jnp.bfloat16
        ),
        "tp",
        scatter_dimension=0,
        tiled=True,
    )
    back = lax.all_to_all(summed, "ep", split_axis=1, concat_axis=1, tiled=True)
    picked = (
        jnp.take(back, slot_index, axis=1).astype(jnp.float32).reshape(-1, row_count, top_count)
    )
    combined = jnp.einsum("drk,rk->rd", picked, route_weights)
    return combined.astype(jnp.bfloat16)


def fits_whole(queries, keys, values, lambdas, tokens, route_ids, w_gate):
    row_count, width = tokens.shape
    ep_size = lax.axis_size("ep")
    tp_size = lax.axis_size("tp")
    expert_count = w_gate.shape[0] * ep_size
    capacity = 2 * row_count * route_ids.shape[1] // expert_count
    return (
        capacity >= row_count
        and w_gate.shape[0] == 1
        and power_of_two(ep_size)
        and ep_size >= 2
        and power_of_two(tp_size)
        and tp_size >= 4
        and row_count % (16 * tp_size) == 0
        and w_gate.shape[2] % 128 == 0
        and width % (128 * tp_size) == 0
        and queries.shape[1] % (128 * lambdas.shape[0]) == 0
        and values.shape[1] % (128 * lambdas.shape[0]) == 0
        and keys.shape[0] % 128 == 0
    )


def on_device(
    queries,
    keys,
    values,
    lambdas,
    head_gain,
    tokens,
    route_ids,
    route_weights,
    moe_gain,
    w_gate,
    w_up,
    w_down,
):
    routed = (tokens, route_ids, route_weights, moe_gain, w_gate, w_up, w_down)
    if fits_whole(queries, keys, values, lambdas, tokens, route_ids, w_gate):
        return whole_rows(queries, keys, values, lambdas, head_gain, *routed)
    heads_out = attend(queries, keys, values, lambdas, head_gain)
    return (heads_out, experts_slots(*routed))


def solution(mesh):
    in_specs = (
        P(("grp", "ep"), "tp"),
        P(("grp", "ep"), "tp"),
        P(("grp", "ep"), "tp"),
        P("tp"),
        P(),
        P(("grp", "ep"), None),
        P(("grp", "ep"), None),
        P(("grp", "ep"), None),
        P(),
        P("ep", None, "tp"),
        P("ep", None, "tp"),
        P("ep", "tp", None),
    )
    out_specs = (P(("grp", "ep"), "tp"), P(("grp", "ep"), "tp"))
    return jax.shard_map(
        on_device, mesh=mesh, in_specs=in_specs, out_specs=out_specs, check_vma=False
    )
```
